32 devices in a mesh: sp: 8 (over z, y), dp: 4 (over x, core).
Axes of the slice: x: 2, y: 2, z: 4, core: 2. Of those that a mesh axis runs over, the one named last changes fastest.
Arguments:
- queries: bfloat16 [4, 1024, 2048], P('dp', 'sp'), may hold values from -40 to 40
- keys: bfloat16 [4, 1024, 512], P('dp', 'sp'), may hold values from -8 to 8
- values: bfloat16 [4, 1024, 512], P('dp', 'sp'), may hold values from -6 to 6
- lambdas: float32 [16], replicated, may hold values from 0.3 to 0.8
- value_gain: float32 [128], replicated, may hold values from 0.1 to 1.9
- out_weight: bfloat16 [2048, 4096], P(None, ('sp', 'dp')), may hold values from -0.125 to 0.125
Outputs:
- mixed: bfloat16 [4, 1024, 4096], P('dp', 'sp')
The draws below stay inside these ranges and needn't reach their ends.
All inputs are finite; a program needn't handle non-finite values.
Results may differ from the reference program's by a relative error of at most 0.0087.
Values may be sent and summed in bfloat16 or wider, within the bound.
A program may use at most 128 MiB of HBM per device.

```python
import jax
import jax.numpy as jnp
from jax import lax

D = 4096
HEADS = 16
KV_HEADS = 4
HEAD_DIM = 64
VALUE_DIM = 128
SEQLEN = 1024
SEQS = 4


def base_keys(key):
    draw_key = jax.random.fold_in(key, 3)
    shape = (SEQS, SEQLEN, KV_HEADS, 2, HEAD_DIM)
    keys_float = jnp.clip(1.3 * jax.random.normal(draw_key, shape, jnp.float32), -8.0, 8.0)
    return keys_float


def draw_keys(key, part):
    return base_keys(key).reshape(SEQS, SEQLEN, KV_HEADS * 2 * HEAD_DIM).astype(jnp.bfloat16)


def draw_queries(key, part):
    draw_key = jax.random.fold_in(key, 4)
    shape = (SEQS, SEQLEN, HEADS, 2, HEAD_DIM)
    queries_float = jnp.clip(1.3 * jax.random.normal(draw_key, shape, jnp.float32), -8.0, 8.0)
    return queries_float.reshape(SEQS, SEQLEN, HEADS * 2 * HEAD_DIM).astype(jnp.bfloat16)


def block_levels(own_key, shape, pieces, low, high):
    loudness = 1.0
    for position, blocks in pieces:
        steps = jax.random.uniform(jax.random.fold_in(jax.random.fold_in(own_key, 6), position), (blocks,), jnp.float32, low / len(pieces), high / len(pieces))
        loudness = loudness * jnp.repeat(jnp.exp(steps), shape[position] // blocks).reshape((-1,) + (1,) * (len(shape) - 1 - position))
    return loudness


def scatter_about(own_key, extent, deviation, most, split=(), kind=jnp.bfloat16):
    result = deviation * jax.random.normal(own_key, extent, jnp.float32)
    if split:
        result = result * block_levels(own_key, extent, split, -0.22, 0.18)
    return jnp.clip(result, -most, most).astype(kind)


def setup_inputs(seed: int = 0) -> dict:
    key_of = jax.random.split(jax.random.key(seed), 7)
    queries = draw_queries(jax.random.fold_in(key_of[6], 71), 0)
    keys = draw_keys(jax.random.fold_in(key_of[6], 71), 0)
    values = scatter_about(key_of[2], (SEQS, SEQLEN, KV_HEADS * VALUE_DIM), 1.0, 6.0, ((0, 4), (1, 8)))
    lambdas = jnp.clip(jax.random.uniform(key_of[3], (HEADS,), jnp.float32, 0.3, 0.8), 0.3, 0.8)
    value_gain = jnp.clip(1.0 + 0.18 * jax.random.normal(key_of[4], (VALUE_DIM,), jnp.float32), 0.1, 1.9)
    out_weight = scatter_about(key_of[5], (HEADS * VALUE_DIM, D), (HEADS * VALUE_DIM) ** -0.5, 0.125, ((1, 32),))
    return {"queries": queries, "keys": keys, "values": values, "lambdas": lambdas, "value_gain": value_gain, "out_weight": out_weight}


rope_base = 500000.0
output_scale = 0.8
norm_eps = 1e-05

def rotate_all(parts, positions):
    width = parts.shape[-1]
    half = width // 2
    freqs = rope_base ** (-jnp.arange(0, width, 2, dtype=jnp.float32) / width)
    angles = positions[:, None] * freqs[None, :]
    shape = (1, angles.shape[0], 1, 1, half)
    cosine = jnp.cos(angles).reshape(shape)
    sine = jnp.sin(angles).reshape(shape)
    first = parts[..., :half]
    second = parts[..., half:]
    return jnp.concatenate([first * cosine - second * sine, second * cosine + first * sine], -1)

def reference(queries, keys, values, lambdas, value_gain, out_weight):
    positions = jnp.arange(SEQLEN, dtype=jnp.float32)
    query_rot = rotate_all(queries.astype(jnp.float32).reshape(SEQS, SEQLEN, HEADS, 2, HEAD_DIM), positions).astype(jnp.bfloat16)
    key_rot = rotate_all(keys.astype(jnp.float32).reshape(SEQS, SEQLEN, KV_HEADS, 2, HEAD_DIM), positions).astype(jnp.bfloat16)
    value_parts = values.reshape(SEQS, SEQLEN, KV_HEADS, VALUE_DIM)
    group_size = HEADS // KV_HEADS
    key_heads = jnp.repeat(key_rot, group_size, axis=2)
    value_heads = jnp.repeat(value_parts, group_size, axis=2)
    query_flat = jnp.transpose(query_rot, (0, 2, 1, 3, 4)).reshape(SEQS * HEADS, SEQLEN, 2, HEAD_DIM)
    key_flat = jnp.transpose(key_heads, (0, 2, 1, 3, 4)).reshape(SEQS * HEADS, SEQLEN, 2, HEAD_DIM)
    value_flat = jnp.transpose(value_heads, (0, 2, 1, 3)).reshape(SEQS * HEADS, SEQLEN, VALUE_DIM)
    lambda_flat = jnp.tile(lambdas, SEQS)
    block_rows = min(512, SEQLEN)
    count = SEQLEN // block_rows
    score_scale = HEAD_DIM ** (-0.5)
    key_places = jnp.arange(SEQLEN)

    def one_head(inputs):
        query_one, key_one, value_one, lambda_one = inputs

        def one_block(block_index):
            start = block_index * block_rows
            query_block = lax.dynamic_slice_in_dim(query_one, start, block_rows, 0)
            scores = jnp.einsum('qmd,kmd->mqk', query_block.astype(jnp.float32), key_one.astype(jnp.float32)) * score_scale
            allowed = key_places[None, :] <= (start + jnp.arange(block_rows))[:, None]
            scores = jnp.where(allowed[None], scores, -jnp.inf)
            row_top = lax.optimization_barrier(jnp.max(scores, -1, keepdims=True))
            raised = jnp.exp(scores - row_top)
            maps = raised / lax.optimization_barrier(jnp.sum(raised, -1, keepdims=True))
            weights = (maps[0] - lambda_one * maps[1]).astype(jnp.bfloat16)
            return jnp.dot(weights, value_one, preferred_element_type=jnp.float32)
        blocks = lax.map(one_block, jnp.arange(count))
        head_values = blocks.reshape(SEQLEN, VALUE_DIM)
        squares = lax.optimization_barrier(jnp.mean(head_values * head_values, -1, keepdims=True))
        return (head_values * lax.rsqrt(squares + norm_eps) * value_gain * output_scale).astype(jnp.bfloat16)
    head_out = lax.map(one_head, (query_flat, key_flat, value_flat, lambda_flat))
    heads_out = jnp.transpose(head_out.reshape(SEQS, HEADS, SEQLEN, VALUE_DIM), (0, 2, 1, 3)).reshape(SEQS * SEQLEN, HEADS * VALUE_DIM)
    mixed = jnp.dot(heads_out, out_weight, preferred_element_type=jnp.float32).astype(jnp.bfloat16)
    return mixed.reshape(SEQS, SEQLEN, D)
```

```python
import functools

import jax
import jax.numpy as jnp
import numpy as np
from jax import lax
from jax.experimental import pallas as pl
from jax.experimental.pallas import tpu as pltpu
from jax.sharding import PartitionSpec as P

HEADS = 16
KV_HEADS = 4
HEAD_DIM = 64
VALUE_DIM = 128
GROUP = HEADS // KV_HEADS
WIDTH = 2 * HEAD_DIM

rope_base = 500000.0
output_scale = 0.8
norm_eps = 1e-05
MESH = pl.DeviceIdType.MESH


def tables(seqlen):
    freqs = rope_base ** (-np.arange(0, HEAD_DIM, 2, dtype=np.float64) / HEAD_DIM)
    angles = np.arange(seqlen, dtype=np.float64)[:, None] * freqs[None, :]
    cosine, sine = np.cos(angles).astype(np.float32), np.sin(angles).astype(np.float32)
    return np.concatenate([cosine] * 4, -1), np.concatenate([-sine, sine, -sine, sine], -1)


def turn(block, cosine, sine):
    half = HEAD_DIM // 2
    lane = lax.broadcasted_iota(jnp.int32, block.shape, 1)
    other = jnp.where(
        lane % HEAD_DIM < half,
        pltpu.roll(block, block.shape[1] - half, 1),
        pltpu.roll(block, half, 1),
    )
    return block * cosine + other * sine


def send(src, dst, send_sem, recv_sem, **device):
    return pltpu.make_async_remote_copy(
        src_ref=src,
        dst_ref=dst,
        send_sem=send_sem,
        recv_sem=recv_sem,
        device_id=device,
        device_id_type=MESH,
    )


def layer_kernel(
    sizes,
    lam_ref,
    q_ref,
    k_ref,
    v_ref,
    cos_ref,
    sin_ref,
    gain_ref,
    w_ref,
    out_ref,
    cos,
    sin,
    q_all,
    kv_own,
    kv_all,
    w_all,
    heads_all,
    built,
    local_sem,
    kvy_send,
    kvy_recv,
    q_send,
    q_recv,
    kvz_send,
    kvz_recv,
    w_send,
    w_recv,
    mate_send,
    mate_recv,
    h_send,
    h_recv,
    o_send,
    o_recv,
):
    bf16 = jnp.bfloat16
    Z, Y, X = sizes
    sp, dp = lax.axis_index("sp"), lax.axis_index("dp")
    z, y = sp // Y, sp % Y
    x, c = dp // 2, dp % 2
    rows = q_ref.shape[0]
    plane = Y * rows
    hpy = KV_HEADS // Y
    own_heads = hpy * GROUP
    span = own_heads * WIDTH
    own = w_ref.shape[1]
    peers = [(kx, ky) for kx in range(X) for ky in range(Y) if kx or ky]

    def place(kx, ky):
        return (x + kx) % X, (y + ky) % Y

    def in_plane(src, dst, sends, recvs, kx, ky):
        to_x, to_y = place(kx, ky)
        return send(src, dst, sends, recvs, sp=z * Y + to_y, dp=to_x * 2 + c)

    def along_z(src, dst, sends, recvs, up):
        to = jnp.minimum(z + 1, Z - 1) if up else jnp.maximum(z - 1, 0)
        return send(src, dst, sends, recvs, sp=to * Y + y)

    has_up, has_down = z < Z - 1, z > 0

    barrier = pltpu.get_barrier_semaphore()
    for kx, ky in peers:
        to_x, to_y = place(kx, ky)
        pl.semaphore_signal(
            barrier, inc=1, device_id={"sp": z * Y + to_y, "dp": to_x * 2 + c}, device_id_type=MESH
        )
    pl.semaphore_signal(barrier, inc=1, device_id={"dp": x * 2 + 1 - c}, device_id_type=MESH)

    @pl.when(has_up)
    def _():
        pl.semaphore_signal(barrier, inc=1, device_id={"sp": sp + Y}, device_id_type=MESH)

    @pl.when(has_down)
    def _():
        pl.semaphore_signal(barrier, inc=1, device_id={"sp": sp - Y}, device_id_type=MESH)

    start_row = pl.multiple_of(z * plane, plane)
    loads = [
        pltpu.make_async_copy(cos_ref.at[pl.ds(start_row, plane)], cos, local_sem.at[0]),
        pltpu.make_async_copy(sin_ref.at[pl.ds(start_row, plane)], sin, local_sem.at[1]),
        pltpu.make_async_copy(w_ref, w_all.at[z, c], local_sem.at[2]),
        pltpu.make_async_copy(
            q_ref.at[:, pl.ds(pl.multiple_of(y * span, span), span)], q_all.at[y], local_sem.at[3]
        ),
    ]
    for copy in loads:
        copy.start()
    loads[0].wait()
    loads[1].wait()
    mine = pl.ds(pl.multiple_of(y * rows, rows), rows)
    for g in range(KV_HEADS):
        cols = slice(g * WIDTH, (g + 1) * WIDTH)
        key = turn(k_ref[:, cols].astype(jnp.float32), cos[mine, :], sin[mine, :])
        kv_own[g, :, :WIDTH] = key.astype(bf16)
        kv_own[g, :, WIDTH:] = v_ref[:, cols]
    for h in range(hpy):
        kv_all[h, z, y] = kv_own[y * hpy + h]

    pl.semaphore_wait(
        barrier, X * Y + has_up.astype(jnp.int32) + has_down.astype(jnp.int32)
    )

    def kvy(h, k):
        to_y = (y + k) % Y
        return in_plane(
            kv_own.at[to_y * hpy + h], kv_all.at[h, z, y], kvy_send.at[k, h], kvy_recv.at[k, h], 0, k
        )

    def qy(h, k):
        to_y = (y + k) % Y
        piece = GROUP * WIDTH
        return in_plane(
            q_ref.at[:, pl.ds(pl.multiple_of((to_y * hpy + h) * piece, piece), piece)],
            q_all.at[y, :, pl.ds(h * piece, piece)],
            q_send.at[k, h],
            q_recv.at[k, h],
            0,
            k,
        )

    def kvz(h, k, k_y):
        at_y = (y - k_y + Y) % Y
        part = kv_all.at[h, jnp.maximum(z - k, 0), at_y]
        return along_z(part, part, kvz_send.at[h, k, k_y], kvz_recv.at[h, k, k_y], True)

    def kvz_wait(h, k, k_y):
        at_y = (y - k_y + Y) % Y
        part = kv_all.at[h, jnp.maximum(z - k, 0), at_y]
        along_z(part, part, kvz_send.at[h, k - 1, k_y], kvz_recv.at[h, k - 1, k_y], True).wait_recv()

    def w_move(up, k):
        piece = w_all.at[jnp.maximum(z - k, 0) if up else jnp.minimum(z + k, Z - 1), c]
        return along_z(piece, piece, w_send.at[int(up), k], w_recv.at[int(up), k], up)

    def w_mate(piece):
        part = w_all.at[piece, c]
        return send(part, part, mate_send.at[piece], mate_recv.at[piece], dp=x * 2 + 1 - c)

    def has_piece(up, k):
        return z >= k if up else z < Z - k

    def piece_of(up, k):
        return jnp.maximum(z - k, 0) if up else jnp.minimum(z + k, Z - 1)

    def w_relay(up, k):
        w_move(up, k - 1).wait_recv()
        w_mate(piece_of(up, k)).start()
        if k < Z - 1:

            @pl.when(has_up if up else has_down)
            def _():
                w_move(up, k).start()

    for h in range(hpy):
        for k in range(1, Y):
            kvy(h, k).start()

        @pl.when(has_up)
        def _():
            kvz(h, 0, 0).start()

    for h in range(hpy):
        for k in range(1, Y):
            qy(h, k).start()
    loads[2].wait()
    w_mate(z).start()

    @pl.when(has_down)
    def _():
        w_move(False, 0).start()

    for h in range(hpy):
        for k in range(1, Y):
            kvy(h, k).wait_recv()

            @pl.when(has_up)
            def _():
                kvz(h, 0, k).start()

    @pl.when(z == 0)
    def _():
        w_move(True, 0).start()

    def kv_relay(h, k):
        for k_y in range(Y):
            kvz_wait(h, k, k_y)
            if k < Z - 1:

                @pl.when(has_up)
                def _():
                    kvz(h, k, k_y).start()

    for k in range(1, Z):

        @pl.when(z >= k)
        def _():
            kv_relay(0, k)

    if hpy == 1:

        @pl.when(has_up & has_down)
        def _():
            w_move(True, 0).start()

    loads[3].wait()
    for k in range(1, Y):
        qy(0, k).wait_recv()

    lane = lax.broadcasted_iota(jnp.int32, (rows, WIDTH), 1)
    below = lax.broadcasted_iota(jnp.int32, (rows, plane), 1) - lax.broadcasted_iota(
        jnp.int32, (rows, plane), 0
    )
    blocks_per_h = GROUP * Y
    nt = (((1,), (1,)), ((), ()))

    def attend(depth, h, local_head, yb):
        query = q_all[yb, :, pl.ds(pl.multiple_of(local_head * WIDTH, WIDTH), WIDTH)]
        at = pl.ds(pl.multiple_of(yb * rows, rows), rows)
        query = turn(query.astype(jnp.float32), cos[at, :], sin[at, :]).astype(bf16)
        query = query.astype(jnp.float32) * HEAD_DIM**-0.5
        allowed = below <= yb * rows
        key = kv_all[h, : depth + 1, :, :, :WIDTH].reshape((depth + 1) * plane, WIDTH)
        value = kv_all[h, : depth + 1, :, :, WIDTH:].reshape((depth + 1) * plane, VALUE_DIM)
        maps = []
        for m in range(2):
            inside = (lane < HEAD_DIM) if m == 0 else (lane >= HEAD_DIM)
            part = jnp.where(inside, query, 0.0).astype(bf16)
            scores = lax.dot_general(part, key, nt, preferred_element_type=jnp.float32)
            last = jnp.where(allowed, scores[:, depth * plane :], -1e30)
            if depth:
                scores = jnp.concatenate([scores[:, : depth * plane], last], -1)
            else:
                scores = last
            raised = jnp.exp(scores - jnp.max(scores, -1, keepdims=True))
            maps.append((raised, jnp.sum(raised, -1, keepdims=True)))
        head = y * own_heads + local_head
        ratio = lam_ref[head] * maps[0][1] / maps[1][1]
        weights = (maps[0][0] - maps[1][0] * ratio).astype(bf16)
        found = jnp.dot(weights, value, preferred_element_type=jnp.float32) / maps[0][1]
        squares = jnp.mean(found * found, -1, keepdims=True)
        normed = found * lax.rsqrt(squares + norm_eps) * gain_ref[...] * output_scale
        at_row = pl.ds(pl.multiple_of(x * plane + yb * rows, rows), rows)
        heads_all[head, at_row, :] = normed.astype(bf16)

    def heads_send(local_head, index):
        kx, ky = peers[index]
        part = heads_all.at[
            y * own_heads + local_head, pl.ds(pl.multiple_of(x * plane, plane), plane)
        ]
        return in_plane(
            part, part, h_send.at[index, local_head], h_recv.at[index, local_head], kx, ky
        )

    def attend_step(i, carry):
        local_head, yb = i // Y, i % Y
        h = i // blocks_per_h
        for other in range(1, hpy):
            for k in range(1, Z):

                @pl.when((i == (other - 1) * blocks_per_h + k - 1) & (z >= k) & has_up)
                def _():
                    kv_relay(other, k)

                @pl.when((i == other * blocks_per_h) & (z >= k) & (z == Z - 1))
                def _():
                    kv_relay(other, k)

            @pl.when(i == other * blocks_per_h)
            def _():
                for k in range(1, Y):
                    qy(other, k).wait_recv()

        if hpy > 1:

            @pl.when((i == (hpy - 2) * blocks_per_h + Z - 1) & has_up & has_down)
            def _():
                w_move(True, 0).start()

        @pl.when((i == own_heads * Y * 5 // 8) & has_up)
        def _():
            w_relay(False, 1)

        for depth in range(Z):

            @pl.when(z == depth)
            def _():
                attend(depth, h, local_head, yb)

        @pl.when(yb == Y - 1)
        def _():
            for index in range(len(peers)):
                heads_send(local_head, index).start()

        return carry

    lax.fori_loop(0, own_heads * Y, attend_step, 0)

    @pl.when(has_down)
    def _():
        w_relay(True, 1)

    for local_head in range(own_heads):
        for index in range(len(peers)):
            heads_send(local_head, index).wait_recv()

    total = X * plane
    tall = min(total, 512)

    def out_send(piece, index):
        kx, ky = peers[index]
        to_x, to_y = place(kx, ky)
        src = built.at[piece, pl.ds(pl.multiple_of(to_x * plane + to_y * rows, rows), rows)]
        return in_plane(
            src, out_at(piece, x, y), o_send.at[piece, index], o_recv.at[piece, index], kx, ky
        )

    def out_at(piece, at_x, at_y):
        block = (piece * Y + at_y) * X + at_x
        if len(out_ref.shape) == 3:
            return out_ref.at[block]
        return out_ref.at[:, pl.ds(pl.multiple_of(block * 2 * own, 2 * own), 2 * own)]

    def project(piece):
        def one(step, carry):
            at = pl.ds(pl.multiple_of(step * tall, tall), tall)
            lhs = jnp.concatenate([heads_all[head, at, :] for head in range(HEADS)], -1)
            if own % 128 == 0:
                rhs = jnp.concatenate([w_all[piece, 0], w_all[piece, 1]], -1)
                built[piece, at, :] = jnp.dot(lhs, rhs, preferred_element_type=jnp.float32).astype(
                    bf16
                )
            else:
                for side in range(2):
                    built[piece, at, side * own : (side + 1) * own] = jnp.dot(
                        lhs, w_all[piece, side], preferred_element_type=jnp.float32
                    ).astype(bf16)
            return carry

        if total == tall:
            one(0, 0)
        else:
            lax.fori_loop(0, total // tall, one, 0)
        for index in range(len(peers)):
            out_send(piece, index).start()
        mine = pl.ds(pl.multiple_of(x * plane + y * rows, rows), rows)
        out_at(piece, x, y)[...] = built[piece, mine, :]

    w_mate(z).wait_recv()
    project(z)
    for k in range(1, Z):
        if k > 1:
            for up in (False, True):

                @pl.when(has_piece(up, k))
                def _():
                    w_relay(up, k)

        for up in (False, True):

            @pl.when(has_piece(up, k))
            def _():
                w_mate(piece_of(up, k)).wait_recv()
                project(piece_of(up, k))

    for piece in range(Z):
        for index in range(len(peers)):
            out_send(piece, index).wait()
    for h in range(hpy):
        for k in range(1, Y):
            kvy(h, k).wait_send()
            qy(h, k).wait_send()
        for k in range(Z - 1):

            @pl.when((z >= k) & has_up)
            def _():
                for k_y in range(Y):
                    kvz(h, k, k_y).wait_send()

    for k in range(Z - 1):

        @pl.when((z >= k) & has_up)
        def _():
            w_move(True, k).wait_send()

        @pl.when((z + k < Z) & has_down)
        def _():
            w_move(False, k).wait_send()

    for piece in range(Z):
        w_mate(piece).wait_send()
    for local_head in range(own_heads):
        for index in range(len(peers)):
            heads_send(local_head, index).wait_send()


def shards(queries, keys, values, lambdas, value_gain, out_weight):
    rows = queries.shape[1]
    sp_count = lax.axis_size("sp")
    dp_count = lax.axis_size("dp")
    X = Y = dp_count // 2
    Z = sp_count // Y
    hpy = KV_HEADS // Y
    own_heads = hpy * GROUP
    vmem = pl.BlockSpec(memory_space=pltpu.VMEM)
    far = pl.BlockSpec(memory_space=pl.ANY)
    bf16 = jnp.bfloat16
    cosine, sine = tables(sp_count * rows)
    depth, own = out_weight.shape
    plane = Y * rows
    blocks = Z * Y * X
    flat = 2 * own % 128 == 0
    shape = (rows, blocks * 2 * own) if flat else (blocks, rows, 2 * own)
    dma = pltpu.SemaphoreType.DMA
    mixed = pl.pallas_call(
        functools.partial(layer_kernel, (Z, Y, X)),
        out_shape=jax.ShapeDtypeStruct(shape, bf16),
        in_specs=[pl.BlockSpec(memory_space=pltpu.SMEM)] + [vmem] * 3 + [far] * 2 + [vmem, far],
        out_specs=vmem,
        scratch_shapes=[
            pltpu.VMEM((plane, WIDTH), jnp.float32),
            pltpu.VMEM((plane, WIDTH), jnp.float32),
            pltpu.VMEM((Y, rows, own_heads * WIDTH), bf16),
            pltpu.VMEM((KV_HEADS, rows, 2 * WIDTH), bf16),
            pltpu.VMEM((hpy, Z, Y, rows, 2 * WIDTH), bf16),
            pltpu.VMEM((Z, 2, depth, own), bf16),
            pltpu.VMEM((HEADS, X * plane, VALUE_DIM), bf16),
            pltpu.VMEM((Z, X * plane, 2 * own), bf16),
            dma((4,)),
        ]
        + [dma((Y, hpy))] * 4
        + [dma((hpy, Z, Y))] * 2
        + [dma((2, Z))] * 2
        + [dma((Z,))] * 2
        + [dma((X * Y - 1, own_heads))] * 2
        + [dma((Z, X * Y - 1))] * 2,
        compiler_params=pltpu.CompilerParams(
            collective_id=0, has_side_effects=True, vmem_limit_bytes=60 * 2**20
        ),
        name="layer",
    )(
        lambdas,
        queries[0],
        keys[0],
        values[0],
        jnp.asarray(cosine),
        jnp.asarray(sine),
        value_gain[None],
        out_weight,
    )
    if not flat:
        mixed = jnp.transpose(mixed, (1, 0, 2)).reshape(rows, -1)
    return mixed[None]


def solution(mesh):
    return jax.shard_map(
        shards,
        mesh=mesh,
        in_specs=(
            P("dp", "sp", None),
            P("dp", "sp", None),
            P("dp", "sp", None),
            P(),
            P(),
            P(None, ("sp", "dp")),
        ),
        out_specs=P("dp", "sp", None),
        check_vma=False,
    )
```

```python
import functools

import jax
import jax.numpy as jnp
import numpy as np
from jax import lax
from jax.experimental import pallas as pl
from jax.experimental.pallas import tpu as pltpu
from jax.sharding import PartitionSpec as P

HEADS = 16
KV_HEADS = 4
HEAD_DIM = 64
VALUE_DIM = 128
GROUP = HEADS // KV_HEADS
WIDTH = 2 * HEAD_DIM

rope_base = 500000.0
output_scale = 0.8
norm_eps = 1e-05
MESH = pl.DeviceIdType.MESH


def tables(seqlen):
    freqs = rope_base ** (-np.arange(0, HEAD_DIM, 2, dtype=np.float64) / HEAD_DIM)
    angles = np.arange(seqlen, dtype=np.float64)[:, None] * freqs[None, :]
    cosine, sine = np.cos(angles).astype(np.float32), np.sin(angles).astype(np.float32)
    return np.concatenate([cosine] * 4, -1), np.concatenate([-sine, sine, -sine, sine], -1)


def turn(block, cosine, sine):
    half = HEAD_DIM // 2
    lane = lax.broadcasted_iota(jnp.int32, block.shape, 1)
    other = jnp.where(
        lane % HEAD_DIM < half,
        pltpu.roll(block, block.shape[1] - half, 1),
        pltpu.roll(block, half, 1),
    )
    return block * cosine + other * sine


def send(src, dst, send_sem, recv_sem, **device):
    return pltpu.make_async_remote_copy(
        src_ref=src,
        dst_ref=dst,
        send_sem=send_sem,
        recv_sem=recv_sem,
        device_id=device,
        device_id_type=MESH,
    )


def layer_kernel(
    sizes,
    lam_ref,
    q_ref,
    k_ref,
    v_ref,
    cos_ref,
    sin_ref,
    gain_ref,
    w_ref,
    out_ref,
    keys,
    values,
    cos,
    sin,
    q_all,
    kv_own,
    kv_all,
    w_all,
    heads_all,
    built,
    local_sem,
    kvy_send,
    kvy_recv,
    q_send,
    q_recv,
    kvz_send,
    kvz_recv,
    w_send,
    w_recv,
    mate_send,
    mate_recv,
    h_send,
    h_recv,
    o_send,
    o_recv,
):
    bf16 = jnp.bfloat16
    Z, Y, X = sizes
    sp, dp = lax.axis_index("sp"), lax.axis_index("dp")
    z, y = sp // Y, sp % Y
    x, c = dp // 2, dp % 2
    rows = q_ref.shape[0]
    plane = Y * rows
    hpy = KV_HEADS // Y
    own_heads = hpy * GROUP
    span = own_heads * WIDTH
    own = w_ref.shape[1]
    peers = [(kx, ky) for kx in range(X) for ky in range(Y) if kx or ky]

    def place(kx, ky):
        return (x + kx) % X, (y + ky) % Y

    def in_plane(src, dst, sends, recvs, kx, ky):
        to_x, to_y = place(kx, ky)
        return send(src, dst, sends, recvs, sp=z * Y + to_y, dp=to_x * 2 + c)

    def along_z(src, dst, sends, recvs, up):
        to = jnp.minimum(z + 1, Z - 1) if up else jnp.maximum(z - 1, 0)
        return send(src, dst, sends, recvs, sp=to * Y + y)

    has_up, has_down = z < Z - 1, z > 0

    start_row = pl.multiple_of(z * plane, plane)
    loads = [
        pltpu.make_async_copy(k_ref, keys, local_sem.at[0]),
        pltpu.make_async_copy(cos_ref.at[pl.ds(start_row, plane)], cos, local_sem.at[1]),
        pltpu.make_async_copy(sin_ref.at[pl.ds(start_row, plane)], sin, local_sem.at[2]),
        pltpu.make_async_copy(v_ref, values, local_sem.at[3]),
        pltpu.make_async_copy(
            q_ref.at[:, pl.ds(pl.multiple_of(y * span, span), span)], q_all.at[y], local_sem.at[4]
        ),
        pltpu.make_async_copy(w_ref, w_all.at[z], local_sem.at[5]),
    ]
    for copy in loads:
        copy.start()

    barrier = pltpu.get_barrier_semaphore()
    for kx in range(X):
        for ky in range(Y):
            to_x, to_y = place(kx, ky)
            for kc in range(2):
                if kx or ky or kc:
                    to = {"sp": z * Y + to_y, "dp": to_x * 2 + (c + kc) % 2}
                    pl.semaphore_signal(barrier, inc=1, device_id=to, device_id_type=MESH)

    @pl.when(has_up)
    def _():
        pl.semaphore_signal(barrier, inc=1, device_id={"sp": sp + Y}, device_id_type=MESH)

    @pl.when(has_down)
    def _():
        pl.semaphore_signal(barrier, inc=1, device_id={"sp": sp - Y}, device_id_type=MESH)

    for copy in loads[:4]:
        copy.wait()
    mine = pl.ds(pl.multiple_of(y * rows, rows), rows)
    for g in range(KV_HEADS):
        cols = slice(g * WIDTH, (g + 1) * WIDTH)
        key = turn(keys[:, cols].astype(jnp.float32), cos[mine, :], sin[mine, :])
        kv_own[g, :, :WIDTH] = key.astype(bf16)
        kv_own[g, :, WIDTH:] = values[:, cols]
    for h in range(hpy):
        kv_all[h, z, y] = kv_own[y * hpy + h]

    pl.semaphore_wait(
        barrier, 2 * X * Y - 1 + has_up.astype(jnp.int32) + has_down.astype(jnp.int32)
    )

    def kvy(h, k):
        to_y = (y + k) % Y
        return in_plane(
            kv_own.at[to_y * hpy + h], kv_all.at[h, z, y], kvy_send.at[k, h], kvy_recv.at[k, h], 0, k
        )

    def qy(h, k):
        to_y = (y + k) % Y
        piece = GROUP * WIDTH
        return in_plane(
            q_ref.at[:, pl.ds(pl.multiple_of((to_y * hpy + h) * piece, piece), piece)],
            q_all.at[y, :, pl.ds(h * piece, piece)],
            q_send.at[k, h],
            q_recv.at[k, h],
            0,
            k,
        )

    def kvz(h, k, k_y):
        at_y = (y - k_y + Y) % Y
        part = kv_all.at[h, jnp.maximum(z - k, 0), at_y]
        return along_z(part, part, kvz_send.at[h, k, k_y], kvz_recv.at[h, k, k_y], True)

    def kvz_wait(h, k, k_y):
        at_y = (y - k_y + Y) % Y
        part = kv_all.at[h, jnp.maximum(z - k, 0), at_y]
        along_z(part, part, kvz_send.at[h, k - 1, k_y], kvz_recv.at[h, k - 1, k_y], True).wait_recv()

    def w_move(up, k):
        piece = w_all.at[piece_of(up, k)]
        return along_z(piece, piece, w_send.at[int(up), k], w_recv.at[int(up), k], up)

    def has_piece(up, k):
        return z >= k if up else z < Z - k

    def piece_of(up, k):
        return jnp.maximum(z - k, 0) if up else jnp.minimum(z + k, Z - 1)

    def w_relay(up, k):
        w_move(up, k - 1).wait_recv()
        if k < Z - 1:

            @pl.when(has_up if up else has_down)
            def _():
                w_move(up, k).start()

    for h in range(hpy):
        for k in range(1, Y):
            kvy(h, k).start()

        @pl.when(has_up)
        def _():
            kvz(h, 0, 0).start()

    for h in range(hpy):
        for k in range(1, Y):
            qy(h, k).start()
    loads[5].wait()

    @pl.when(has_down)
    def _():
        w_move(False, 0).start()

    for h in range(hpy):
        for k in range(1, Y):
            kvy(h, k).wait_recv()

            @pl.when(has_up)
            def _():
                kvz(h, 0, k).start()

    @pl.when(z == 0)
    def _():
        w_move(True, 0).start()

    def kv_relay(h, k):
        for k_y in range(Y):
            kvz_wait(h, k, k_y)
            if k < Z - 1:

                @pl.when(has_up)
                def _():
                    kvz(h, k, k_y).start()

    for k in range(1, Z):

        @pl.when(z >= k)
        def _():
            kv_relay(0, k)

    if hpy == 1:

        @pl.when(has_up & has_down)
        def _():
            w_move(True, 0).start()

    loads[4].wait()
    for k in range(1, Y):
        qy(0, k).wait_recv()

    lane = lax.broadcasted_iota(jnp.int32, (rows, WIDTH), 1)
    below = lax.broadcasted_iota(jnp.int32, (rows, plane), 1) - lax.broadcasted_iota(
        jnp.int32, (rows, plane), 0
    )
    blocks_per_h = GROUP * Y
    nt = (((1,), (1,)), ((), ()))

    def attend(depth, h, local_head, yb):
        query = q_all[yb, :, pl.ds(pl.multiple_of(local_head * WIDTH, WIDTH), WIDTH)]
        at = pl.ds(pl.multiple_of(yb * rows, rows), rows)
        query = turn(query.astype(jnp.float32), cos[at, :], sin[at, :]).astype(bf16)
        query = query.astype(jnp.float32) * HEAD_DIM**-0.5
        allowed = below <= yb * rows
        key = kv_all[h, : depth + 1, :, :, :WIDTH].reshape((depth + 1) * plane, WIDTH)
        value = kv_all[h, : depth + 1, :, :, WIDTH:].reshape((depth + 1) * plane, VALUE_DIM)
        maps = []
        for m in range(2):
            inside = (lane < HEAD_DIM) if m == 0 else (lane >= HEAD_DIM)
            part = jnp.where(inside, query, 0.0).astype(bf16)
            scores = lax.dot_general(part, key, nt, preferred_element_type=jnp.float32)
            last = jnp.where(allowed, scores[:, depth * plane :], -1e30)
            if depth:
                scores = jnp.concatenate([scores[:, : depth * plane], last], -1)
            else:
                scores = last
            raised = jnp.exp(scores - jnp.max(scores, -1, keepdims=True))
            maps.append((raised, jnp.sum(raised, -1, keepdims=True)))
        head = y * own_heads + local_head
        ratio = lam_ref[head] * maps[0][1] / maps[1][1]
        weights = (maps[0][0] - maps[1][0] * ratio).astype(bf16)
        found = jnp.dot(weights, value, preferred_element_type=jnp.float32) / maps[0][1]
        squares = jnp.mean(found * found, -1, keepdims=True)
        normed = found * lax.rsqrt(squares + norm_eps) * gain_ref[...] * output_scale
        at_row = pl.ds(pl.multiple_of(dp * plane + yb * rows, rows), rows)
        heads_all[head, at_row, :] = normed.astype(bf16)

    def heads_send(local_head, index):
        kx, ky = peers[index]
        part = heads_all.at[
            y * own_heads + local_head, pl.ds(pl.multiple_of(dp * plane, plane), plane)
        ]
        return in_plane(
            part, part, h_send.at[index], h_recv.at[index, local_head], kx, ky
        )

    def heads_mate(local_head, index):
        kx, ky = peers[index] if index < len(peers) else (0, 0)
        from_x, from_y = (x - kx + X) % X, (y - ky + Y) % Y
        at = pl.ds(pl.multiple_of((from_x * 2 + c) * plane, plane), plane)
        part = heads_all.at[from_y * own_heads + local_head, at]
        return send(part, part, mate_send.at[index], mate_recv.at[index], dp=x * 2 + 1 - c)

    def attend_step(i, carry):
        local_head, yb = i // Y, i % Y
        h = i // blocks_per_h
        for other in range(1, hpy):
            for k in range(1, Z):

                @pl.when((i == (other - 1) * blocks_per_h + k - 1) & (z >= k) & has_up)
                def _():
                    kv_relay(other, k)

                @pl.when((i == other * blocks_per_h) & (z >= k) & (z == Z - 1))
                def _():
                    kv_relay(other, k)

            @pl.when(i == other * blocks_per_h)
            def _():
                for k in range(1, Y):
                    qy(other, k).wait_recv()

        if hpy > 1:

            @pl.when((i == (hpy - 2) * blocks_per_h + Z - 1) & has_up & has_down)
            def _():
                w_move(True, 0).start()

        @pl.when((i == own_heads * Y * 5 // 8) & has_up)
        def _():
            w_relay(False, 1)

        for depth in range(Z):

            @pl.when(z == depth)
            def _():
                attend(depth, h, local_head, yb)

        @pl.when(yb == Y - 1)
        def _():
            for index in range(len(peers)):
                heads_send(local_head, index).start()
            heads_mate(local_head, len(peers)).start()

        return carry

    lax.fori_loop(0, own_heads * Y, attend_step, 0)

    def relay_if(up, k, extra=True):
        if k < Z:

            @pl.when(has_piece(up, k) & extra)
            def _():
                w_relay(up, k)

    all_chunks = heads_all.at[pl.ds(0, own_heads), pl.ds(0, plane)]

    def chunks_done(sem):
        pltpu.make_async_copy(all_chunks, all_chunks, sem).wait()

    relay_if(True, 1)
    relay_if(False, 2)
    for local_head in range(own_heads):
        for index in range(len(peers)):
            heads_send(local_head, index).wait_recv()
            heads_mate(local_head, index).start()
    relay_if(True, 2, has_up)
    for index in range(len(peers) + 1):
        chunks_done(mate_recv.at[index])

    def out_at(piece, at_x, at_y, at_c):
        block = ((piece * Y + at_y) * X + at_x) * 2 + at_c
        if len(out_ref.shape) == 3:
            return out_ref.at[block]
        return out_ref.at[:, pl.ds(pl.multiple_of(block * own, own), own)]

    def out_send(piece, kx, ky, kc):
        to_x, to_y = place(kx, ky)
        to_c = (c + kc) % 2
        start = pl.multiple_of((to_x * 2 + to_c) * plane + to_y * rows, rows)
        return send(
            built.at[piece, pl.ds(start, rows)],
            out_at(piece, x, y, c),
            o_send,
            o_recv,
            sp=z * Y + to_y,
            dp=to_x * 2 + to_c,
        )

    def project(piece):
        def one(step, carry):
            kx = (step + 1) % X
            tall = 2 * plane
            at = pl.ds(pl.multiple_of((x + kx) % X * tall, tall), tall)
            lhs = jnp.concatenate([heads_all[head, at, :] for head in range(HEADS)], -1)
            found = jnp.dot(lhs, w_all[piece], preferred_element_type=jnp.float32)
            built[piece, at, :] = found.astype(bf16)
            for ky in reversed(range(Y)):
                for kc in reversed(range(2)):
                    if ky or kc:
                        out_send(piece, kx, ky, kc).start()
                    else:

                        @pl.when(kx > 0)
                        def _():
                            out_send(piece, kx, 0, 0).start()

            return carry

        lax.fori_loop(0, X, one, 0)
        mine = pl.ds(pl.multiple_of(dp * plane + y * rows, rows), rows)
        out_at(piece, x, y, c)[...] = built[piece, mine, :]

    def finish_sends():
        for h in range(hpy):
            for k in range(1, Y):
                kvy(h, k).wait_send()
                qy(h, k).wait_send()
            for k in range(Z - 1):

                @pl.when((z >= k) & has_up)
                def _():
                    for k_y in range(Y):
                        kvz(h, k, k_y).wait_send()

        for index in range(len(peers)):
            chunks_done(h_send.at[index])
        for index in range(len(peers) + 1):
            chunks_done(mate_send.at[index])
        for k in range(Z - 1):

            @pl.when((z + k < Z) & has_down)
            def _():
                w_move(False, k).wait_send()

    project(z)
    for k in range(1, Z):
        if k > 2:
            relay_if(False, k)
        if k == Z - 1:
            finish_sends()
        if k == 2:
            relay_if(True, k, ~has_up)
        elif k > 2:
            relay_if(True, k)
        for up in (False, True):

            @pl.when(has_piece(up, k))
            def _():
                project(piece_of(up, k))

    others = built.at[:, pl.ds(0, (2 * X * Y - 1) * rows)]
    pltpu.make_async_copy(others, others, o_recv).wait()
    pltpu.make_async_copy(others, others, o_send).wait()
    for k in range(Z - 1):

        @pl.when((z >= k) & has_up)
        def _():
            w_move(True, k).wait_send()


def shards(queries, keys, values, lambdas, value_gain, out_weight):
    rows = queries.shape[1]
    sp_count = lax.axis_size("sp")
    dp_count = lax.axis_size("dp")
    X = Y = dp_count // 2
    Z = sp_count // Y
    hpy = KV_HEADS // Y
    own_heads = hpy * GROUP
    vmem = pl.BlockSpec(memory_space=pltpu.VMEM)
    far = pl.BlockSpec(memory_space=pltpu.HBM)
    bf16 = jnp.bfloat16
    cosine, sine = tables(sp_count * rows)
    depth, own = out_weight.shape
    plane = Y * rows
    blocks = Z * Y * X * 2
    flat = own % 128 == 0
    shape = (rows, blocks * own) if flat else (blocks, rows, own)
    dma = pltpu.SemaphoreType.DMA
    mixed = pl.pallas_call(
        functools.partial(layer_kernel, (Z, Y, X)),
        out_shape=pltpu.VMEM(shape, bf16),
        in_specs=[pl.BlockSpec(memory_space=pltpu.SMEM)] + [far] * 5 + [vmem, far],
        out_specs=vmem,
        scratch_shapes=[
            pltpu.VMEM((rows, KV_HEADS * WIDTH), bf16),
            pltpu.VMEM((rows, KV_HEADS * VALUE_DIM), bf16),
            pltpu.VMEM((plane, WIDTH), jnp.float32),
            pltpu.VMEM((plane, WIDTH), jnp.float32),
            pltpu.VMEM((Y, rows, own_heads * WIDTH), bf16),
            pltpu.VMEM((KV_HEADS, rows, 2 * WIDTH), bf16),
            pltpu.VMEM((hpy, Z, Y, rows, 2 * WIDTH), bf16),
            pltpu.VMEM((Z, depth, own), bf16),
            pltpu.VMEM((HEADS, 2 * X * plane, VALUE_DIM), bf16),
            pltpu.VMEM((Z, 2 * X * plane, own), bf16),
            dma((6,)),
        ]
        + [dma((Y, hpy))] * 4
        + [dma((hpy, Z, Y))] * 2
        + [dma((2, Z))] * 2
        + [dma((X * Y,))] * 2
        + [dma((X * Y - 1,)), dma((X * Y - 1, own_heads))]
        + [dma(())] * 2,
        compiler_params=pltpu.CompilerParams(
            collective_id=0, has_side_effects=True, vmem_limit_bytes=40 * 2**20
        ),
        name="layer",
    )(
        pltpu.with_memory_space_constraint(lambdas, pltpu.HBM),
        pltpu.with_memory_space_constraint(queries[0], pltpu.HBM),
        pltpu.with_memory_space_constraint(keys[0], pltpu.HBM),
        pltpu.with_memory_space_constraint(values[0], pltpu.HBM),
        pltpu.with_memory_space_constraint(jnp.asarray(cosine), pltpu.HBM),
        pltpu.with_memory_space_constraint(jnp.asarray(sine), pltpu.HBM),
        pltpu.with_memory_space_constraint(value_gain[None], pltpu.HBM),
        pltpu.with_memory_space_constraint(out_weight, pltpu.HBM),
    )
    if not flat:
        mixed = jnp.transpose(mixed, (1, 0, 2)).reshape(rows, -1)
    return mixed[None]


def solution(mesh):
    return jax.shard_map(
        shards,
        mesh=mesh,
        in_specs=(
            P("dp", "sp", None),
            P("dp", "sp", None),
            P("dp", "sp", None),
            P(),
            P(),
            P(None, ("sp", "dp")),
        ),
        out_specs=P("dp", "sp", None),
        check_vma=False,
    )
```

```python
import functools

import jax
import jax.numpy as jnp
import numpy as np
from jax import lax
from jax.experimental import pallas as pl
from jax.experimental.pallas import tpu as pltpu
from jax.sharding import PartitionSpec as P

HEADS = 16
KV_HEADS = 4
HEAD_DIM = 64
VALUE_DIM = 128
GROUP = HEADS // KV_HEADS
WIDTH = 2 * HEAD_DIM

rope_base = 500000.0
output_scale = 0.8
norm_eps = 1e-05
MESH = pl.DeviceIdType.MESH


def tables(seqlen):
    freqs = rope_base ** (-np.arange(0, HEAD_DIM, 2, dtype=np.float64) / HEAD_DIM)
    angles = np.arange(seqlen, dtype=np.float64)[:, None] * freqs[None, :]
    cosine, sine = np.cos(angles).astype(np.float32), np.sin(angles).astype(np.float32)
    return np.concatenate([cosine] * 4, -1), np.concatenate([-sine, sine, -sine, sine], -1)


def turn(block, cosine, sine):
    half = HEAD_DIM // 2
    lane = lax.broadcasted_iota(jnp.int32, block.shape, 1)
    other = jnp.where(
        lane % HEAD_DIM < half,
        pltpu.roll(block, block.shape[1] - half, 1),
        pltpu.roll(block, half, 1),
    )
    return block * cosine + other * sine


def send(src, dst, send_sem, recv_sem, **device):
    return pltpu.make_async_remote_copy(
        src_ref=src,
        dst_ref=dst,
        send_sem=send_sem,
        recv_sem=recv_sem,
        device_id=device,
        device_id_type=MESH,
    )


def layer_kernel(
    sizes,
    lam_ref,
    q_ref,
    k_ref,
    v_ref,
    cos_ref,
    sin_ref,
    gain_ref,
    w_ref,
    out_ref,
    keys,
    values,
    cos,
    sin,
    q_all,
    kv_own,
    kv_all,
    w_all,
    heads_all,
    heads_up,
    built,
    local_sem,
    kvy_send,
    kvy_recv,
    q_send,
    q_recv,
    kvt_send,
    kvt_recv,
    qt_send,
    qt_recv,
    hz_send,
    hz_recv,
    kvz_send,
    kvz_recv,
    w_send,
    w_recv,
    mate_send,
    mate_recv,
    h_send,
    h_recv,
    o_send,
    o_recv,
):
    bf16 = jnp.bfloat16
    Z, Y, X = sizes
    sp, dp = lax.axis_index("sp"), lax.axis_index("dp")
    z, y = sp // Y, sp % Y
    x, c = dp // 2, dp % 2
    rows = q_ref.shape[0]
    plane = Y * rows
    hpy = KV_HEADS // Y
    own_heads = hpy * GROUP
    span = own_heads * WIDTH
    own = w_ref.shape[1]
    peers = [(kx, ky) for kx in range(X) for ky in range(Y) if kx or ky]

    def place(kx, ky):
        return (x + kx) % X, (y + ky) % Y

    def in_plane(src, dst, sends, recvs, kx, ky):
        to_x, to_y = place(kx, ky)
        return send(src, dst, sends, recvs, sp=z * Y + to_y, dp=to_x * 2 + c)

    def along_z(src, dst, sends, recvs, up):
        to = jnp.minimum(z + 1, Z - 1) if up else jnp.maximum(z - 1, 0)
        return send(src, dst, sends, recvs, sp=to * Y + y)

    has_up, has_down = z < Z - 1, z > 0
    top, helper, kv_up = z == Z - 1, z == Z - 2, z < Z - 2
    parts = 4

    first = jnp.minimum(z, Z - 2)
    start_row = pl.multiple_of(first * plane, plane)
    loads = [
        pltpu.make_async_copy(k_ref, keys, local_sem.at[0]),
        pltpu.make_async_copy(cos_ref.at[pl.ds(start_row, 2 * plane)], cos, local_sem.at[1]),
        pltpu.make_async_copy(sin_ref.at[pl.ds(start_row, 2 * plane)], sin, local_sem.at[2]),
        pltpu.make_async_copy(v_ref, values, local_sem.at[3]),
        pltpu.make_async_copy(
            q_ref.at[:, pl.ds(pl.multiple_of(y * span, span), span)], q_all.at[0, y], local_sem.at[4]
        ),
        pltpu.make_async_copy(w_ref, w_all.at[z], local_sem.at[5]),
    ]
    for copy in loads:
        copy.start()

    barrier = pltpu.get_barrier_semaphore()
    for kx in range(X):
        for ky in range(Y):
            to_x, to_y = place(kx, ky)
            for kc in range(2):
                if kx or ky or kc:
                    to = {"sp": z * Y + to_y, "dp": to_x * 2 + (c + kc) % 2}
                    pl.semaphore_signal(barrier, inc=1, device_id=to, device_id_type=MESH)

    @pl.when(has_up)
    def _():
        pl.semaphore_signal(barrier, inc=1, device_id={"sp": sp + Y}, device_id_type=MESH)

    @pl.when(has_down)
    def _():
        pl.semaphore_signal(barrier, inc=1, device_id={"sp": sp - Y}, device_id_type=MESH)

    for copy in loads[:4]:
        copy.wait()
    mine = pl.ds(pl.multiple_of((z - first) * plane + y * rows, rows), rows)
    for g in range(KV_HEADS):
        cols = slice(g * WIDTH, (g + 1) * WIDTH)
        key = turn(keys[:, cols].astype(jnp.float32), cos[mine, :], sin[mine, :])
        kv_own[g, :, :WIDTH] = key.astype(bf16)
        kv_own[g, :, WIDTH:] = values[:, cols]
    for h in range(hpy):
        kv_all[h, z, y] = kv_own[y * hpy + h]

    near = has_up.astype(jnp.int32) + has_down.astype(jnp.int32)
    pl.semaphore_wait(barrier, 2 * X * Y - 1 + near)

    def kvy(h, k):
        to_y = (y + k) % Y
        return in_plane(
            kv_own.at[to_y * hpy + h], kv_all.at[h, z, y], kvy_send, kvy_recv.at[k - 1, h], 0, k
        )

    def qy(h, k):
        to_y = (y + k) % Y
        piece = GROUP * WIDTH
        return in_plane(
            q_ref.at[:, pl.ds(pl.multiple_of((to_y * hpy + h) * piece, piece), piece)],
            q_all.at[0, y, :, pl.ds(h * piece, piece)],
            q_send,
            q_recv.at[k - 1, h],
            0,
            k,
        )

    def kvt(h, k):
        part = kv_all.at[h, Z - 1, (y - k + Y) % Y]
        return send(part, part, kvt_send, kvt_recv.at[h], sp=(Z - 2) * Y + y)

    def qt(h, k):
        piece = GROUP * WIDTH
        at_y = (y - k + Y) % Y
        cols = pl.ds(h * piece, piece)
        return send(
            q_all.at[0, at_y, :, cols],
            q_all.at[1, at_y, :, cols],
            qt_send,
            qt_recv.at[h],
            sp=(Z - 2) * Y + y,
        )

    def hz(local_head):
        return send(
            heads_up.at[local_head],
            heads_part(local_head, 0, 0),
            hz_send,
            hz_recv.at[local_head],
            sp=(Z - 1) * Y + y,
        )

    def kvz(h, k, k_y):
        at_y = (y - k_y + Y) % Y
        part = kv_all.at[h, jnp.maximum(z - k, 0), at_y]
        return along_z(part, part, kvz_send, kvz_recv.at[h, k, k_y], True)

    def kvz_wait(h, k, k_y):
        at_y = (y - k_y + Y) % Y
        part = kv_all.at[h, jnp.maximum(z - k, 0), at_y]
        along_z(part, part, kvz_send, kvz_recv.at[h, k - 1, k_y], True).wait_recv()

    def w_move(up, k, part):
        cut = w_all.shape[1] // parts
        piece = w_all.at[piece_of(up, k), pl.ds(part * cut, cut)]
        side = int(up)
        return along_z(piece, piece, w_send.at[side], w_recv.at[side, k, part], up)

    def has_piece(up, k):
        return z >= k if up else z < Z - k

    def piece_of(up, k):
        return jnp.maximum(z - k, 0) if up else jnp.minimum(z + k, Z - 1)

    def w_relay(up, k, part):
        w_move(up, k - 1, part).wait_recv()
        if k < Z - 1:

            @pl.when(has_up if up else has_down)
            def _():
                w_move(up, k, part).start()

    def w_own(up, some=range(4)):
        for part in some:
            w_move(up, 0, part).start()

    middle = has_up & has_down

    for h in range(hpy):
        for k in range(1, Y):
            kvy(h, k).start()

        @pl.when(kv_up if h == 0 else z == 0)
        def _():
            kvz(h, 0, 0).start()

        for k in range(1, Y):
            qy(h, k).start()

    @pl.when(helper)
    def _():
        loads[5].wait()
        w_own(True)

    for k in range(1, Y):
        kvy(0, k).wait_recv()

        @pl.when(kv_up)
        def _():
            kvz(0, 0, k).start()

    @pl.when(top)
    def _():
        loads[4].wait()
        for h in range(hpy):
            for k in range(Y):
                if k and h:
                    kvy(h, k).wait_recv()
                if k:
                    qy(h, k).wait_recv()
                kvt(h, k).start()
                qt(h, k).start()

    @pl.when(~helper)
    def _():
        loads[5].wait()

    @pl.when(has_down)
    def _():
        w_own(False)

    def late_kv(h):
        for k in range(1, Y):
            kvy(h, k).wait_recv()

    @pl.when(z == 0)
    def _():
        for h in range(1, hpy):
            late_kv(h)
            for k in range(1, Y):
                kvz(h, 0, k).start()

    if Z > 2:

        @pl.when(z == 0)
        def _():
            w_own(True)

    def kv_relay(h, k):
        for k_y in range(Y):
            kvz_wait(h, k, k_y)
            if k < Z - 2:

                @pl.when(kv_up)
                def _():
                    kvz(h, k, k_y).start()

    for k in range(1, Z - 1):

        @pl.when((z >= k) & has_up)
        def _():
            kv_relay(0, k)

    @pl.when(kv_up & has_down)
    def _():
        w_own(True, range(2))
        for h in range(1, hpy):
            late_kv(h)
            for k in range(Y):
                kvz(h, 0, k).start()
        if hpy == 1:
            w_own(True, range(2, 4))

    @pl.when(has_up)
    def _():
        loads[4].wait()
        for k in range(1, Y):
            qy(0, k).wait_recv()

    def done(ref, sem):
        pltpu.make_async_copy(ref, ref, sem).wait()

    def take_top(h):
        done(kv_all.at[h, Z - 1], kvt_recv.at[h])
        done(q_all.at[1, :, :, pl.ds(h * GROUP * WIDTH, GROUP * WIDTH)], qt_recv.at[h])

    lane = lax.broadcasted_iota(jnp.int32, (plane, WIDTH), 1)
    allowed = lax.broadcasted_iota(jnp.int32, (plane, plane), 1) <= lax.broadcasted_iota(
        jnp.int32, (plane, plane), 0
    )
    nt = (((1,), (1,)), ((), ()))
    lag = 2
    direct = own_heads - 2

    def attend(depth, h, local_head, above=0):
        at = pl.ds(pl.multiple_of(local_head * WIDTH, WIDTH), WIDTH)
        query = q_all[above, :, :, at].reshape(plane, WIDTH)
        table = pl.ds(above * plane, plane)
        query = turn(query.astype(jnp.float32), cos[table, :], sin[table, :]).astype(bf16)
        query = query.astype(jnp.float32) * HEAD_DIM**-0.5
        key = kv_all[h, : depth + 1, :, :, :WIDTH].reshape((depth + 1) * plane, WIDTH)
        value = kv_all[h, : depth + 1, :, :, WIDTH:].reshape((depth + 1) * plane, VALUE_DIM)
        maps = []
        for m in range(2):
            inside = (lane < HEAD_DIM) if m == 0 else (lane >= HEAD_DIM)
            part = jnp.where(inside, query, 0.0).astype(bf16)
            scores = lax.dot_general(part, key, nt, preferred_element_type=jnp.float32)
            last = jnp.where(allowed, scores[:, depth * plane :], -1e30)
            if depth:
                scores = jnp.concatenate([scores[:, : depth * plane], last], -1)
            else:
                scores = last
            raised = jnp.exp(scores - jnp.max(scores, -1, keepdims=True))
            maps.append((raised, jnp.sum(raised, -1, keepdims=True)))
        head = y * own_heads + local_head
        ratio = lam_ref[head] * maps[0][1] / maps[1][1]
        weights = (maps[0][0] - maps[1][0] * ratio).astype(bf16)
        found = jnp.dot(weights, value, preferred_element_type=jnp.float32) / maps[0][1]
        squares = jnp.mean(found * found, -1, keepdims=True)
        normed = found * lax.rsqrt(squares + norm_eps) * gain_ref[...] * output_scale
        if above:
            heads_up[local_head] = normed.astype(bf16)
        else:
            at_row = pl.ds(pl.multiple_of(dp * plane, plane), plane)
            heads_all[head, at_row, :] = normed.astype(bf16)

    def heads_part(local_head, kx, ky):
        from_x, from_y = (x - kx + X) % X, (y - ky + Y) % Y
        at = pl.ds(pl.multiple_of((from_x * 2 + c) * plane, plane), plane)
        return heads_all.at[from_y * own_heads + local_head, at]

    def heads_send(local_head, to, start=(0, 0)):
        index = peers.index(to)
        part = heads_part(local_head, *start)
        hop = (to[0] - start[0], to[1] - start[1])
        return in_plane(part, part, h_send.at[index], h_recv.at[index, local_head], *hop)

    straight = [peer for peer in peers if not (peer[0] and peer[1])]
    corners = [peer for peer in peers if peer[0] and peer[1]]

    def heads_relay(local_head):
        for peer in straight:
            heads_send(local_head, peer).wait_recv()
            heads_mate(local_head, peer).start()
            parity = 0 if peer[0] else 1

            @pl.when((local_head % 2 == parity) & (local_head < direct))
            def _():
                for corner in corners:
                    if corner[parity] == peer[parity]:
                        heads_send(local_head, corner, peer).start()

    def heads_mate(local_head, peer):
        index = peers.index(peer) if peer in peers else len(peers)
        part = heads_part(local_head, *peer)
        return send(part, part, mate_send.at[index], mate_recv.at[index], dp=x * 2 + 1 - c)

    def attend_step(i, carry):
        h = i // GROUP
        for other in range(1, hpy):
            for k in range(1, Z - 1):

                @pl.when((i == (other - 1) * GROUP + k - 1) & (z >= k) & kv_up)
                def _():
                    kv_relay(other, k)

            @pl.when((i == other * GROUP) & has_up)
            def _():
                for k in range(1, Y):
                    qy(other, k).wait_recv()

        if hpy > 1:

            @pl.when((i == (hpy - 2) * GROUP + Z - 3) & kv_up & has_down)
            def _():
                w_own(True, range(2, 4))

        for up, k, part, step, where in in_loop:

            @pl.when((i == step) & where)
            def _():
                w_relay(up, k, part)

        for depth in range(Z - 1):

            @pl.when(z == depth)
            def _():
                attend(depth, h, i)

        @pl.when(top)
        def _():
            hz(i).wait_recv()

        for peer in straight:
            heads_send(i, peer).start()
        heads_mate(i, (0, 0)).start()

        @pl.when(i >= direct)
        def _():
            for peer in corners:
                heads_send(i, peer).start()

        @pl.when(i >= lag)
        def _():
            heads_relay(i - lag)

        @pl.when(helper & (i == GROUP - 1))
        def _():
            for other in range(hpy):
                if other:
                    late_kv(other)
                    for k in range(1, Z - 1):

                        @pl.when(z >= k)
                        def _():
                            kv_relay(other, k)

                for up, k, part, step, where in in_loop:
                    if step == slots + other:
                        w_relay(up, k, part)
                take_top(other)

                def above_step(j, carry):
                    attend(Z - 1, other, j, 1)
                    hz(j).start()
                    return carry

                lax.fori_loop(other * GROUP, (other + 1) * GROUP, above_step, 0)

        return carry

    slots = own_heads
    in_loop = []
    if slots >= 8 and Z > 3:
        for part in range(parts):
            in_loop.append((True, 1, part, 3 + part, middle & ~helper))
            in_loop.append((False, 1, part, 2 + part, middle & ~helper))
            in_loop.append((True, 1, part, (3, slots + 1, 4, 5)[part], helper))
        for part in range(2):
            in_loop.append((False, 1, part, 5 + 2 * part, helper))
        in_loop.append((True, 2, 0, 7, helper))
    lax.fori_loop(0, own_heads, attend_step, 0)

    def relay_rest(up, k, part):
        done = z < 0
        for up_, k_, part_, _, where in in_loop:
            if (up_, k_, part_) == (up, k, part):
                done = done | where
        return ~done & has_piece(up, k)

    def relay_if(up, k, where, some=range(4)):
        if k >= Z:
            return
        for part in some:

            @pl.when(relay_rest(up, k, part) & where)
            def _():
                w_relay(up, k, part)

    all_chunks = heads_all.at[pl.ds(0, own_heads), pl.ds(0, plane)]

    def chunks_done(sem):
        pltpu.make_async_copy(all_chunks, all_chunks, sem).wait()

    relay_if(True, 1, middle)
    relay_if(True, 2, helper & has_down, range(2))
    for local_head in range(own_heads - lag, own_heads):
        heads_relay(jnp.int32(local_head))
    relay_if(False, 1, middle)
    relay_if(True, 2, helper & has_down, range(2, 3))
    for local_head in range(own_heads):
        for peer in corners:
            heads_send(local_head, peer).wait_recv()
            heads_mate(local_head, peer).start()
        if local_head == own_heads // 2:
            relay_if(True, 2, helper & has_down, range(3, 4))
    for index in range(len(peers) + 1):
        chunks_done(mate_recv.at[index])

    def out_at(piece, at_x, at_y, at_c):
        block = ((piece * Y + at_y) * X + at_x) * 2 + at_c
        if len(out_ref.shape) == 3:
            return out_ref.at[block]
        return out_ref.at[:, pl.ds(pl.multiple_of(block * own, own), own)]

    def out_send(piece, kx, ky, kc):
        to_x, to_y = place(kx, ky)
        to_c = (c + kc) % 2
        start = pl.multiple_of((to_x * 2 + to_c) * plane + to_y * rows, rows)
        return send(
            built.at[piece, pl.ds(start, rows)],
            out_at(piece, x, y, c),
            o_send,
            o_recv,
            sp=z * Y + to_y,
            dp=to_x * 2 + to_c,
        )

    def project(piece):
        def one(step, carry):
            kx = (step + 1) % X
            tall = 2 * plane
            at = pl.ds(pl.multiple_of((x + kx) % X * tall, tall), tall)
            lhs = jnp.concatenate([heads_all[head, at, :] for head in range(HEADS)], -1)
            found = jnp.dot(lhs, w_all[piece], preferred_element_type=jnp.float32)
            built[piece, at, :] = found.astype(bf16)
            for ky in reversed(range(Y)):
                for kc in reversed(range(2)):
                    if ky or kc:
                        out_send(piece, kx, ky, kc).start()
                    else:

                        @pl.when(kx > 0)
                        def _():
                            out_send(piece, kx, 0, 0).start()

            return carry

        lax.fori_loop(0, X, one, 0)
        mine = pl.ds(pl.multiple_of(dp * plane + y * rows, rows), rows)
        out_at(piece, x, y, c)[...] = built[piece, mine, :]

    def finish_sends():
        if Y > 1:
            done(kv_own.at[pl.ds(0, hpy * (Y - 1))], kvy_send)
            done(q_all.at[0, pl.ds(0, Y - 1)], q_send)

        @pl.when(top)
        def _():
            done(kv_own, kvt_send)
            done(q_all.at[0], qt_send)

        @pl.when(helper)
        def _():
            done(heads_up, hz_send)

        for depth in range(Z - 2):

            @pl.when(z == depth)
            def _():
                done(kv_all.at[:, pl.ds(0, depth + 1)], kvz_send)

        for index in range(len(peers)):
            chunks_done(h_send.at[index])
        for index in range(len(peers) + 1):
            chunks_done(mate_send.at[index])
        for depth in range(1, Z):

            @pl.when(z == depth)
            def _():
                done(w_all.at[pl.ds(0, Z - depth)], w_send.at[0])

    inner = middle & ~helper

    def project_if(up, k):
        @pl.when(has_piece(up, k))
        def _():
            project(piece_of(up, k))

    relay_if(False, 2, inner, range(1))
    project(z)
    relay_if(False, 2, inner, range(1, 2))
    for k in range(1, Z):
        if k == Z - 1:
            finish_sends()
        relay_if(False, k, ~middle if k < 3 else z >= 0)
        relay_if(True, k, ~middle if k == 1 else ~(helper & has_down) if k == 2 else z >= 0)
        project_if(False, k)
        if k == 1:
            relay_if(False, 2, inner, range(2, 3))
        project_if(True, k)
        if k == 1:
            relay_if(False, 2, inner, range(3, 4))

    others = built.at[:, pl.ds(0, (2 * X * Y - 1) * rows)]
    pltpu.make_async_copy(others, others, o_recv).wait()
    pltpu.make_async_copy(others, others, o_send).wait()
    for depth in range(Z - 1):

        @pl.when(z == depth)
        def _():
            done(w_all.at[pl.ds(0, depth + 1)], w_send.at[1])


def shards(queries, keys, values, lambdas, value_gain, out_weight):
    rows = queries.shape[1]
    sp_count = lax.axis_size("sp")
    dp_count = lax.axis_size("dp")
    X = Y = dp_count // 2
    Z = sp_count // Y
    hpy = KV_HEADS // Y
    own_heads = hpy * GROUP
    vmem = pl.BlockSpec(memory_space=pltpu.VMEM)
    far = pl.BlockSpec(memory_space=pltpu.HBM)
    bf16 = jnp.bfloat16
    cosine, sine = tables(sp_count * rows)
    depth, own = out_weight.shape
    plane = Y * rows
    blocks = Z * Y * X * 2
    flat = own % 128 == 0
    shape = (rows, blocks * own) if flat else (blocks, rows, own)
    dma = pltpu.SemaphoreType.DMA
    mixed = pl.pallas_call(
        functools.partial(layer_kernel, (Z, Y, X)),
        out_shape=pltpu.VMEM(shape, bf16),
        in_specs=[pl.BlockSpec(memory_space=pltpu.SMEM)] + [far] * 5 + [vmem, far],
        out_specs=vmem,
        scratch_shapes=[
            pltpu.VMEM((rows, KV_HEADS * WIDTH), bf16),
            pltpu.VMEM((rows, KV_HEADS * VALUE_DIM), bf16),
            pltpu.VMEM((2 * plane, WIDTH), jnp.float32),
            pltpu.VMEM((2 * plane, WIDTH), jnp.float32),
            pltpu.VMEM((2, Y, rows, own_heads * WIDTH), bf16),
            pltpu.VMEM((KV_HEADS, rows, 2 * WIDTH), bf16),
            pltpu.VMEM((hpy, Z, Y, rows, 2 * WIDTH), bf16),
            pltpu.VMEM((Z, depth, own), bf16),
            pltpu.VMEM((HEADS, 2 * X * plane, VALUE_DIM), bf16),
            pltpu.VMEM((own_heads, plane, VALUE_DIM), bf16),
            pltpu.VMEM((Z, 2 * X * plane, own), bf16),
            dma((6,)),
        ]
        + [dma(()), dma((Y - 1, hpy))] * 2
        + [dma(()), dma((hpy,))] * 2
        + [dma(()), dma((own_heads,))]
        + [dma(()), dma((hpy, max(Z - 2, 1), Y))]
        + [dma((2,)), dma((2, Z - 1, 4))]
        + [dma((X * Y,))] * 2
        + [dma((X * Y - 1,)), dma((X * Y - 1, own_heads))]
        + [dma(())] * 2,
        compiler_params=pltpu.CompilerParams(
            collective_id=0, has_side_effects=True, vmem_limit_bytes=40 * 2**20
        ),
        name="layer",
    )(
        pltpu.with_memory_space_constraint(lambdas, pltpu.HBM),
        pltpu.with_memory_space_constraint(queries[0], pltpu.HBM),
        pltpu.with_memory_space_constraint(keys[0], pltpu.HBM),
        pltpu.with_memory_space_constraint(values[0], pltpu.HBM),
        pltpu.with_memory_space_constraint(jnp.asarray(cosine), pltpu.HBM),
        pltpu.with_memory_space_constraint(jnp.asarray(sine), pltpu.HBM),
        pltpu.with_memory_space_constraint(value_gain[None], pltpu.HBM),
        pltpu.with_memory_space_constraint(out_weight, pltpu.HBM),
    )
    if not flat:
        mixed = jnp.transpose(mixed, (1, 0, 2)).reshape(rows, -1)
    return mixed[None]


def solution(mesh):
    return jax.shard_map(
        shards,
        mesh=mesh,
        in_specs=(
            P("dp", "sp", None),
            P("dp", "sp", None),
            P("dp", "sp", None),
            P(),
            P(),
            P(None, ("sp", "dp")),
        ),
        out_specs=P("dp", "sp", None),
        check_vma=False,
    )
```

```python
import functools

import jax
import jax.numpy as jnp
import numpy as np
from jax import lax
from jax.experimental import pallas as pl
from jax.experimental.pallas import tpu as pltpu
from jax.sharding import PartitionSpec as P

HEADS = 16
KV_HEADS = 4
HEAD_DIM = 64
VALUE_DIM = 128
GROUP = HEADS // KV_HEADS
WIDTH = 2 * HEAD_DIM

rope_base = 500000.0
output_scale = 0.8
norm_eps = 1e-05
MESH = pl.DeviceIdType.MESH


def tables(seqlen):
    freqs = rope_base ** (-np.arange(0, HEAD_DIM, 2, dtype=np.float64) / HEAD_DIM)
    angles = np.arange(seqlen, dtype=np.float64)[:, None] * freqs[None, :]
    cosine, sine = np.cos(angles).astype(np.float32), np.sin(angles).astype(np.float32)
    return np.concatenate([cosine] * 4, -1), np.concatenate([-sine, sine, -sine, sine], -1)


def turn(block, cosine, sine):
    half = HEAD_DIM // 2
    lane = lax.broadcasted_iota(jnp.int32, block.shape, 1)
    other = jnp.where(
        lane % HEAD_DIM < half,
        pltpu.roll(block, block.shape[1] - half, 1),
        pltpu.roll(block, half, 1),
    )
    return block * cosine + other * sine


def send(src, dst, send_sem, recv_sem, **device):
    return pltpu.make_async_remote_copy(
        src_ref=src,
        dst_ref=dst,
        send_sem=send_sem,
        recv_sem=recv_sem,
        device_id=device,
        device_id_type=MESH,
    )


def layer_kernel(
    sizes,
    lam_ref,
    q_ref,
    k_ref,
    v_ref,
    cos_ref,
    sin_ref,
    gain_ref,
    w_ref,
    out_ref,
    keys,
    values,
    cos,
    sin,
    q_all,
    kv_own,
    kv_all,
    w_all,
    heads_all,
    heads_up,
    built,
    local_sem,
    kvy_send,
    kvy_recv,
    q_send,
    q_recv,
    kvt_send,
    kvt_recv,
    qt_send,
    qt_recv,
    hz_send,
    hz_recv,
    kvz_send,
    kvz_recv,
    w_send,
    w_recv,
    mate_send,
    mate_recv,
    h_send,
    h_recv,
    o_send,
    o_recv,
):
    bf16 = jnp.bfloat16
    Z, Y, X = sizes
    sp, dp = lax.axis_index("sp"), lax.axis_index("dp")
    z, y = sp // Y, sp % Y
    x, c = dp // 2, dp % 2
    rows = q_ref.shape[0]
    plane = Y * rows
    hpy = KV_HEADS // Y
    own_heads = hpy * GROUP
    span = own_heads * WIDTH
    own = w_ref.shape[1]
    peers = [(kx, ky) for kx in range(X) for ky in range(Y) if kx or ky]

    def place(kx, ky):
        return (x + kx) % X, (y + ky) % Y

    def in_plane(src, dst, sends, recvs, kx, ky):
        to_x, to_y = place(kx, ky)
        return send(src, dst, sends, recvs, sp=z * Y + to_y, dp=to_x * 2 + c)

    def along_z(src, dst, sends, recvs, up):
        to = jnp.minimum(z + 1, Z - 1) if up else jnp.maximum(z - 1, 0)
        return send(src, dst, sends, recvs, sp=to * Y + y)

    has_up, has_down = z < Z - 1, z > 0
    top, helper, kv_up = z == Z - 1, z == Z - 2, z < Z - 2
    parts = 4
    moved = max(1, hpy // 2)

    first = jnp.minimum(z, Z - 2)
    start_row = pl.multiple_of(first * plane, plane)
    loads = [
        pltpu.make_async_copy(k_ref, keys, local_sem.at[0]),
        pltpu.make_async_copy(cos_ref.at[pl.ds(start_row, 2 * plane)], cos, local_sem.at[1]),
        pltpu.make_async_copy(sin_ref.at[pl.ds(start_row, 2 * plane)], sin, local_sem.at[2]),
        pltpu.make_async_copy(v_ref, values, local_sem.at[3]),
        pltpu.make_async_copy(
            q_ref.at[:, pl.ds(pl.multiple_of(y * span, span), span)], q_all.at[0, y], local_sem.at[4]
        ),
        pltpu.make_async_copy(w_ref, w_all.at[z], local_sem.at[5]),
    ]
    for copy in loads:
        copy.start()

    barrier = pltpu.get_barrier_semaphore()
    for kx in range(X):
        for ky in range(Y):
            to_x, to_y = place(kx, ky)
            for kc in range(2):
                if kx or ky or kc:
                    to = {"sp": z * Y + to_y, "dp": to_x * 2 + (c + kc) % 2}
                    pl.semaphore_signal(barrier, inc=1, device_id=to, device_id_type=MESH)

    @pl.when(has_up)
    def _():
        pl.semaphore_signal(barrier, inc=1, device_id={"sp": sp + Y}, device_id_type=MESH)

    @pl.when(has_down)
    def _():
        pl.semaphore_signal(barrier, inc=1, device_id={"sp": sp - Y}, device_id_type=MESH)

    for copy in loads[:4]:
        copy.wait()
    mine = pl.ds(pl.multiple_of((z - first) * plane + y * rows, rows), rows)
    for g in range(KV_HEADS):
        cols = slice(g * WIDTH, (g + 1) * WIDTH)
        key = turn(keys[:, cols].astype(jnp.float32), cos[mine, :], sin[mine, :])
        kv_own[g, :, :WIDTH] = key.astype(bf16)
        kv_own[g, :, WIDTH:] = values[:, cols]
    for h in range(hpy):
        kv_all[h, z, y] = kv_own[y * hpy + h]

    near = has_up.astype(jnp.int32) + has_down.astype(jnp.int32)
    pl.semaphore_wait(barrier, 2 * X * Y - 1 + near)

    def kvy(h, k):
        to_y = (y + k) % Y
        return in_plane(
            kv_own.at[to_y * hpy + h], kv_all.at[h, z, y], kvy_send, kvy_recv.at[k - 1, h], 0, k
        )

    def qy(h, k):
        to_y = (y + k) % Y
        piece = GROUP * WIDTH
        return in_plane(
            q_ref.at[:, pl.ds(pl.multiple_of((to_y * hpy + h) * piece, piece), piece)],
            q_all.at[0, y, :, pl.ds(h * piece, piece)],
            q_send,
            q_recv.at[k - 1, h],
            0,
            k,
        )

    def kvt(h, k):
        part = kv_all.at[h, Z - 1, (y - k + Y) % Y]
        return send(part, part, kvt_send, kvt_recv.at[h], sp=(Z - 2) * Y + y)

    def qt(h, k):
        piece = GROUP * WIDTH
        at_y = (y - k + Y) % Y
        cols = pl.ds(h * piece, piece)
        return send(
            q_all.at[0, at_y, :, cols],
            q_all.at[1, at_y, :, cols],
            qt_send,
            qt_recv.at[h],
            sp=(Z - 2) * Y + y,
        )

    def hz(local_head):
        return send(
            heads_up.at[local_head],
            heads_part(local_head, 0, 0),
            hz_send,
            hz_recv.at[local_head],
            sp=(Z - 1) * Y + y,
        )

    def kvz(h, k, k_y):
        at_y = (y - k_y + Y) % Y
        part = kv_all.at[h, jnp.maximum(z - k, 0), at_y]
        return along_z(part, part, kvz_send, kvz_recv.at[h, k, k_y], True)

    def kvz_wait(h, k, k_y):
        at_y = (y - k_y + Y) % Y
        part = kv_all.at[h, jnp.maximum(z - k, 0), at_y]
        along_z(part, part, kvz_send, kvz_recv.at[h, k - 1, k_y], True).wait_recv()

    def w_move(up, k, part):
        cut = w_all.shape[1] // parts
        piece = w_all.at[piece_of(up, k), pl.ds(part * cut, cut)]
        side = int(up)
        return along_z(piece, piece, w_send.at[side], w_recv.at[side, k, part], up)

    def has_piece(up, k):
        return z >= k if up else z < Z - k

    def piece_of(up, k):
        return jnp.maximum(z - k, 0) if up else jnp.minimum(z + k, Z - 1)

    def w_relay(up, k, part):
        w_move(up, k - 1, part).wait_recv()
        if k < Z - 1:

            @pl.when(has_up if up else has_down)
            def _():
                w_move(up, k, part).start()

    def w_own(up, some=range(4)):
        for part in some:
            w_move(up, 0, part).start()

    middle = has_up & has_down

    for h in range(hpy):
        for k in range(1, Y):
            kvy(h, k).start()

        @pl.when(kv_up if h == 0 else kv_up & (z == 0))
        def _():
            kvz(h, 0, 0).start()

        for k in range(1, Y):
            qy(h, k).start()

    @pl.when(helper)
    def _():
        loads[5].wait()
        w_own(True, range(3) if moved < hpy else range(4))

    for k in range(1, Y):
        kvy(0, k).wait_recv()

        @pl.when(kv_up)
        def _():
            kvz(0, 0, k).start()

    @pl.when(top)
    def _():
        loads[4].wait()
        for h in range(moved):
            for k in range(Y):
                if k and h:
                    kvy(h, k).wait_recv()
                if k:
                    qy(h, k).wait_recv()
                kvt(h, k).start()
                qt(h, k).start()

    @pl.when(~helper)
    def _():
        loads[5].wait()

    @pl.when(has_down)
    def _():
        w_own(False)

    def late_kv(h):
        for k in range(1, Y):
            kvy(h, k).wait_recv()

    @pl.when(kv_up & (z == 0))
    def _():
        for h in range(1, hpy):
            late_kv(h)
            for k in range(1, Y):
                kvz(h, 0, k).start()

    if Z > 2:

        @pl.when(kv_up & (z == 0))
        def _():
            w_own(True)

    def kv_relay(h, k):
        for k_y in range(Y):
            kvz_wait(h, k, k_y)
            if k < (Z - 1 if h >= moved else Z - 2):

                @pl.when(has_up if h >= moved else kv_up)
                def _():
                    kvz(h, k, k_y).start()

    for k in range(1, Z - 1):

        @pl.when((z >= k) & has_up)
        def _():
            kv_relay(0, k)

    @pl.when(kv_up & has_down)
    def _():
        for h in range(1, hpy):
            late_kv(h)
            for k in range(Y):
                kvz(h, 0, k).start()
        if hpy == 1:
            w_own(True)

    @pl.when(helper)
    def _():
        for h in range(1, hpy):
            late_kv(h)
            if h >= moved:
                for k in range(Y):
                    kvz(h, 0, k).start()

    @pl.when(has_up)
    def _():
        loads[4].wait()
        for k in range(1, Y):
            qy(0, k).wait_recv()

    def done(ref, sem):
        pltpu.make_async_copy(ref, ref, sem).wait()

    def take_top(h):
        done(kv_all.at[h, Z - 1], kvt_recv.at[h])
        done(q_all.at[1, :, :, pl.ds(h * GROUP * WIDTH, GROUP * WIDTH)], qt_recv.at[h])

    lane = lax.broadcasted_iota(jnp.int32, (plane, WIDTH), 1)
    allowed = lax.broadcasted_iota(jnp.int32, (plane, plane), 1) <= lax.broadcasted_iota(
        jnp.int32, (plane, plane), 0
    )
    nt = (((1,), (1,)), ((), ()))
    lag = 2
    direct = own_heads - 2

    def attend(depth, h, local_head, above=0, table=0):
        at = pl.ds(pl.multiple_of(local_head * WIDTH, WIDTH), WIDTH)
        query = q_all[above, :, :, at].reshape(plane, WIDTH)
        table = pl.ds(table * plane, plane)
        query = turn(query.astype(jnp.float32), cos[table, :], sin[table, :]).astype(bf16)
        query = query.astype(jnp.float32) * HEAD_DIM**-0.5
        key = kv_all[h, : depth + 1, :, :, :WIDTH].reshape((depth + 1) * plane, WIDTH)
        value = kv_all[h, : depth + 1, :, :, WIDTH:].reshape((depth + 1) * plane, VALUE_DIM)
        maps = []
        for m in range(2):
            inside = (lane < HEAD_DIM) if m == 0 else (lane >= HEAD_DIM)
            part = jnp.where(inside, query, 0.0).astype(bf16)
            scores = lax.dot_general(part, key, nt, preferred_element_type=jnp.float32)
            last = jnp.where(allowed, scores[:, depth * plane :], -1e30)
            if depth:
                scores = jnp.concatenate([scores[:, : depth * plane], last], -1)
            else:
                scores = last
            raised = jnp.exp(scores - jnp.max(scores, -1, keepdims=True))
            maps.append((raised, jnp.sum(raised, -1, keepdims=True)))
        head = y * own_heads + local_head
        ratio = lam_ref[head] * maps[0][1] / maps[1][1]
        weights = (maps[0][0] - maps[1][0] * ratio).astype(bf16)
        found = jnp.dot(weights, value, preferred_element_type=jnp.float32) / maps[0][1]
        squares = jnp.mean(found * found, -1, keepdims=True)
        normed = found * lax.rsqrt(squares + norm_eps) * gain_ref[...] * output_scale
        if above:
            heads_up[local_head] = normed.astype(bf16)
        else:
            at_row = pl.ds(pl.multiple_of(dp * plane, plane), plane)
            heads_all[head, at_row, :] = normed.astype(bf16)

    def heads_part(local_head, kx, ky):
        from_x, from_y = (x - kx + X) % X, (y - ky + Y) % Y
        at = pl.ds(pl.multiple_of((from_x * 2 + c) * plane, plane), plane)
        return heads_all.at[from_y * own_heads + local_head, at]

    def heads_send(local_head, to, start=(0, 0)):
        index = peers.index(to)
        part = heads_part(local_head, *start)
        hop = (to[0] - start[0], to[1] - start[1])
        return in_plane(part, part, h_send.at[index], h_recv.at[index, local_head], *hop)

    straight = [peer for peer in peers if not (peer[0] and peer[1])]
    corners = [peer for peer in peers if peer[0] and peer[1]]

    kept = (hpy - moved) * GROUP

    def order(position):
        return jnp.where(top, (position + moved * GROUP) % own_heads, position)

    def heads_relay(position):
        local_head = order(position)
        for peer in straight:
            heads_send(local_head, peer).wait_recv()
            heads_mate(local_head, peer).start()
            parity = 0 if peer[0] else 1

            @pl.when((position % 2 == parity) & (position < direct))
            def _():
                for corner in corners:
                    if corner[parity] == peer[parity]:
                        heads_send(local_head, corner, peer).start()

    def heads_mate(local_head, peer):
        index = peers.index(peer) if peer in peers else len(peers)
        part = heads_part(local_head, *peer)
        return send(part, part, mate_send.at[index], mate_recv.at[index], dp=x * 2 + 1 - c)

    def attend_step(i, carry):
        head = order(i)
        h = head // GROUP
        for other in range(1, hpy):
            for k in range(1, Z - 1):

                @pl.when((i == (other - 1) * GROUP + k - 1) & (z >= k) & kv_up)
                def _():
                    kv_relay(other, k)

                if other >= moved:

                    @pl.when((i == min(k + 1, GROUP - 1)) & (z >= k) & helper)
                    def _():
                        kv_relay(other, k)

            if other >= moved:

                @pl.when((i == (other - moved) * GROUP) & top)
                def _():
                    late_kv(other)
                    for k in range(1, Z):
                        kv_relay(other, k)
                    for k in range(1, Y):
                        qy(other, k).wait_recv()

            @pl.when((i == other * GROUP) & has_up)
            def _():
                for k in range(1, Y):
                    qy(other, k).wait_recv()

        if hpy > 1:

            @pl.when((i == (hpy - 2) * GROUP + Z - 3) & kv_up & has_down)
            def _():
                w_own(True)

            if moved < hpy:

                @pl.when((i == GROUP) & helper)
                def _():
                    w_own(True, range(3, 4))

        for up, k, part, step, where in in_loop:

            @pl.when((i == step) & where)
            def _():
                w_relay(up, k, part)

        for depth in range(Z - 1):

            @pl.when(z == depth)
            def _():
                attend(depth, h, head)

        @pl.when(top & (i >= kept))
        def _():
            hz(head).wait_recv()

        if moved < hpy:

            @pl.when(top & (i < kept))
            def _():
                attend(Z - 1, h, head, 0, 1)

        for peer in straight:
            heads_send(head, peer).start()
        heads_mate(head, (0, 0)).start()

        @pl.when(i >= direct)
        def _():
            for peer in corners:
                heads_send(head, peer).start()

        @pl.when(i >= lag)
        def _():
            heads_relay(i - lag)

        @pl.when(helper & (i == GROUP - 1))
        def _():
            for other in range(moved):
                if other:
                    for k in range(1, Z - 1):

                        @pl.when(z >= k)
                        def _():
                            kv_relay(other, k)

                for up, k, part, step, where in in_loop:
                    if step == slots + other:
                        w_relay(up, k, part)
                take_top(other)

                def above_step(j, carry):
                    attend(Z - 1, other, j, 1, 1)
                    hz(j).start()
                    return carry

                lax.fori_loop(other * GROUP, (other + 1) * GROUP, above_step, 0)

        return carry

    slots = own_heads
    in_loop = []
    if slots >= 8 and Z > 3:
        for part in range(parts):
            in_loop.append((True, 1, part, 3 + part, middle & ~helper))
            in_loop.append((False, 1, part, 2 + part, middle & ~helper))
            if part < 3:
                in_loop.append((True, 1, part, (4, 5, 7)[part], helper))
        for part in range(2):
            in_loop.append((False, 1, part, 6 + part, helper))
    lax.fori_loop(0, own_heads, attend_step, 0)

    def relay_rest(up, k, part):
        done = z < 0
        for up_, k_, part_, _, where in in_loop:
            if (up_, k_, part_) == (up, k, part):
                done = done | where
        return ~done & has_piece(up, k)

    def relay_if(up, k, where, some=range(4)):
        if k >= Z:
            return
        for part in some:

            @pl.when(relay_rest(up, k, part) & where)
            def _():
                w_relay(up, k, part)

    all_chunks = heads_all.at[pl.ds(0, own_heads), pl.ds(0, plane)]

    def chunks_done(sem):
        pltpu.make_async_copy(all_chunks, all_chunks, sem).wait()

    relay_if(True, 1, middle)
    relay_if(True, 2, helper & has_down, range(2))
    for local_head in range(own_heads - lag, own_heads):
        heads_relay(jnp.int32(local_head))
    relay_if(False, 1, middle)
    relay_if(True, 2, helper & has_down, range(2, 3))
    for local_head in range(own_heads):
        for peer in corners:
            heads_send(local_head, peer).wait_recv()
            heads_mate(local_head, peer).start()
        if local_head == own_heads // 2:
            relay_if(True, 2, helper & has_down, range(3, 4))
    for index in range(len(peers) + 1):
        chunks_done(mate_recv.at[index])

    def out_at(piece, at_x, at_y, at_c):
        block = ((piece * Y + at_y) * X + at_x) * 2 + at_c
        if len(out_ref.shape) == 3:
            return out_ref.at[block]
        return out_ref.at[:, pl.ds(pl.multiple_of(block * own, own), own)]

    def out_send(piece, kx, ky, kc):
        to_x, to_y = place(kx, ky)
        to_c = (c + kc) % 2
        start = pl.multiple_of((to_x * 2 + to_c) * plane + to_y * rows, rows)
        return send(
            built.at[piece, pl.ds(start, rows)],
            out_at(piece, x, y, c),
            o_send,
            o_recv,
            sp=z * Y + to_y,
            dp=to_x * 2 + to_c,
        )

    def project(piece):
        def one(step, carry):
            kx = (step + 1) % X
            tall = 2 * plane
            at = pl.ds(pl.multiple_of((x + kx) % X * tall, tall), tall)
            lhs = jnp.concatenate([heads_all[head, at, :] for head in range(HEADS)], -1)
            found = jnp.dot(lhs, w_all[piece], preferred_element_type=jnp.float32)
            built[piece, at, :] = found.astype(bf16)
            for ky in reversed(range(Y)):
                for kc in reversed(range(2)):
                    if ky or kc:
                        out_send(piece, kx, ky, kc).start()
                    else:

                        @pl.when(kx > 0)
                        def _():
                            out_send(piece, kx, 0, 0).start()

            return carry

        lax.fori_loop(0, X, one, 0)
        mine = pl.ds(pl.multiple_of(dp * plane + y * rows, rows), rows)
        out_at(piece, x, y, c)[...] = built[piece, mine, :]

    def finish_sends():
        if Y > 1:
            done(kv_own.at[pl.ds(0, hpy * (Y - 1))], kvy_send)
            done(q_all.at[0, pl.ds(0, Y - 1)], q_send)

        @pl.when(top)
        def _():
            done(kv_own.at[pl.ds(0, moved * Y)], kvt_send)
            done(q_all.at[0, :, :, pl.ds(0, moved * GROUP * WIDTH)], qt_send)

        @pl.when(helper)
        def _():
            done(heads_up, hz_send)

        for depth in range(Z - 2):

            @pl.when(z == depth)
            def _():
                done(kv_all.at[:, pl.ds(0, depth + 1)], kvz_send)

        if moved < hpy:

            @pl.when(helper)
            def _():
                done(kv_all.at[pl.ds(moved, hpy - moved), pl.ds(0, Z - 1)], kvz_send)

        for index in range(len(peers)):
            chunks_done(h_send.at[index])
        for index in range(len(peers) + 1):
            chunks_done(mate_send.at[index])
        for depth in range(1, Z):

            @pl.when(z == depth)
            def _():
                done(w_all.at[pl.ds(0, Z - depth)], w_send.at[0])

    inner = middle & ~helper

    def project_if(up, k):
        @pl.when(has_piece(up, k))
        def _():
            project(piece_of(up, k))

    relay_if(False, 2, inner, range(1))
    project(z)
    relay_if(False, 2, inner, range(1, 2))
    for k in range(1, Z):
        if k == Z - 1:
            finish_sends()
        relay_if(False, k, ~middle if k < 3 else z >= 0)
        relay_if(True, k, ~middle if k == 1 else ~(helper & has_down) if k == 2 else z >= 0)
        project_if(False, k)
        if k == 1:
            relay_if(False, 2, inner, range(2, 3))
        project_if(True, k)
        if k == 1:
            relay_if(False, 2, inner, range(3, 4))

    others = built.at[:, pl.ds(0, (2 * X * Y - 1) * rows)]
    pltpu.make_async_copy(others, others, o_recv).wait()
    pltpu.make_async_copy(others, others, o_send).wait()
    for depth in range(Z - 1):

        @pl.when(z == depth)
        def _():
            done(w_all.at[pl.ds(0, depth + 1)], w_send.at[1])


def shards(queries, keys, values, lambdas, value_gain, out_weight):
    rows = queries.shape[1]
    sp_count = lax.axis_size("sp")
    dp_count = lax.axis_size("dp")
    X = Y = dp_count // 2
    Z = sp_count // Y
    hpy = KV_HEADS // Y
    own_heads = hpy * GROUP
    moved = max(1, hpy // 2)
    vmem = pl.BlockSpec(memory_space=pltpu.VMEM)
    far = pl.BlockSpec(memory_space=pltpu.HBM)
    bf16 = jnp.bfloat16
    cosine, sine = tables(sp_count * rows)
    depth, own = out_weight.shape
    plane = Y * rows
    blocks = Z * Y * X * 2
    flat = own % 128 == 0
    shape = (rows, blocks * own) if flat else (blocks, rows, own)
    dma = pltpu.SemaphoreType.DMA
    mixed = pl.pallas_call(
        functools.partial(layer_kernel, (Z, Y, X)),
        out_shape=pltpu.VMEM(shape, bf16),
        in_specs=[pl.BlockSpec(memory_space=pltpu.SMEM)] + [far] * 5 + [vmem, far],
        out_specs=vmem,
        scratch_shapes=[
            pltpu.VMEM((rows, KV_HEADS * WIDTH), bf16),
            pltpu.VMEM((rows, KV_HEADS * VALUE_DIM), bf16),
            pltpu.VMEM((2 * plane, WIDTH), jnp.float32),
            pltpu.VMEM((2 * plane, WIDTH), jnp.float32),
            pltpu.VMEM((2, Y, rows, own_heads * WIDTH), bf16),
            pltpu.VMEM((KV_HEADS, rows, 2 * WIDTH), bf16),
            pltpu.VMEM((hpy, Z, Y, rows, 2 * WIDTH), bf16),
            pltpu.VMEM((Z, depth, own), bf16),
            pltpu.VMEM((HEADS, 2 * X * plane, VALUE_DIM), bf16),
            pltpu.VMEM((moved * GROUP, plane, VALUE_DIM), bf16),
            pltpu.VMEM((Z, 2 * X * plane, own), bf16),
            dma((6,)),
        ]
        + [dma(()), dma((Y - 1, hpy))] * 2
        + [dma(()), dma((moved,))] * 2
        + [dma(()), dma((moved * GROUP,))]
        + [dma(()), dma((hpy, Z - 1, Y))]
        + [dma((2,)), dma((2, Z - 1, 4))]
        + [dma((X * Y,))] * 2
        + [dma((X * Y - 1,)), dma((X * Y - 1, own_heads))]
        + [dma(())] * 2,
        compiler_params=pltpu.CompilerParams(
            collective_id=0, has_side_effects=True, vmem_limit_bytes=40 * 2**20
        ),
        name="layer",
    )(
        pltpu.with_memory_space_constraint(lambdas, pltpu.HBM),
        pltpu.with_memory_space_constraint(queries[0], pltpu.HBM),
        pltpu.with_memory_space_constraint(keys[0], pltpu.HBM),
        pltpu.with_memory_space_constraint(values[0], pltpu.HBM),
        pltpu.with_memory_space_constraint(jnp.asarray(cosine), pltpu.HBM),
        pltpu.with_memory_space_constraint(jnp.asarray(sine), pltpu.HBM),
        pltpu.with_memory_space_constraint(value_gain[None], pltpu.HBM),
        pltpu.with_memory_space_constraint(out_weight, pltpu.HBM),
    )
    if not flat:
        mixed = jnp.transpose(mixed, (1, 0, 2)).reshape(rows, -1)
    return mixed[None]


def solution(mesh):
    return jax.shard_map(
        shards,
        mesh=mesh,
        in_specs=(
            P("dp", "sp", None),
            P("dp", "sp", None),
            P("dp", "sp", None),
            P(),
            P(),
            P(None, ("sp", "dp")),
        ),
        out_specs=P("dp", "sp", None),
        check_vma=False,
    )
```
